32 devices in a mesh: ep: 16 (over z, y, x), tp: 2 (over core).
Axes of the slice: x: 2, y: 2, z: 4, core: 2. Of those that a mesh axis runs over, the one named last changes fastest.
Arguments:
- tokens: bfloat16 [4096, 2048], P('ep', 'tp'), may hold values from -6 to 6
- experts: int32 [4096, 16], P('ep'), may hold values from 0 to 65535, as said below
- weights: float32 [4096, 16], P('ep'), may hold values from 0.05 to 1
- up_table: bfloat16 [65536, 2048], P('ep', 'tp'), may hold values from -0.125 to 0.125
- out_table: bfloat16 [65536, 2048], P('ep', 'tp')
- gain: float32 [2048], P('tp'), may hold values from 0.1 to 1.9
Outputs:
- normed: bfloat16 [4096, 2048], P('ep', 'tp')
The draws below stay inside these ranges and needn't reach their ends.
Inputs may be any that keep to these rules, and one draw needn't show every extreme that they name: An expert number e lies with index e // 4096 of ep. Among the rows of one index of ep, at most 512 chosen experts lie with any one index of ep, and in every draw some index of ep receives exactly 512 from every index.
All inputs are finite; a program needn't handle non-finite values.
Results may differ from the reference program's by a relative error of at most 0.006.
Values may be sent and summed in bfloat16 or wider, within the bound.
A program may use at most 128 MiB of HBM per device.

```python
import math
import jax
import jax.numpy as jnp
from jax import lax

D = 2048
SLOTS = 16
EXPERTS_PER_RANK = 4096
TOK_DEV = 256
TOKENS = 4096
EXPERTS = 65536
ROW_LIMIT = 512
N_EP = 16


def draw_experts(key, part):
    request_list = TOK_DEV * SLOTS
    slot_count = N_EP * ROW_LIMIT
    order = jax.random.permutation(jax.random.fold_in(key, 11), N_EP)
    pinned_choice = (order < N_EP // 8).astype(jnp.int32)
    slot_holder_rank = jnp.arange(slot_count, dtype=jnp.int32) // ROW_LIMIT

    def one_source(sender_rank):
        score_key = jax.random.fold_in(key, sender_rank + 100)
        random_jitter = jax.random.randint(jax.random.fold_in(score_key, 1), (slot_count,), 0, 4096, dtype=jnp.int32)
        expert_score = (pinned_choice[slot_holder_rank] * 8192 + random_jitter) * slot_count + jnp.arange(slot_count, dtype=jnp.int32)
        selected_rows = lax.top_k(expert_score, request_list)[1].astype(jnp.int32)
        owner_ranks = jax.random.permutation(jax.random.fold_in(score_key, 2), selected_rows // ROW_LIMIT)
        picked_experts = jax.random.randint(jax.random.fold_in(score_key, 3), (3, request_list), 0, EXPERTS_PER_RANK, dtype=jnp.int32)
        local = picked_experts[0] * picked_experts[1] // EXPERTS_PER_RANK * picked_experts[2] // EXPERTS_PER_RANK
        return (owner_ranks * EXPERTS_PER_RANK + local).reshape(TOK_DEV, SLOTS)
    return lax.map(one_source, jnp.arange(N_EP, dtype=jnp.int32)).reshape(TOK_DEV * N_EP, SLOTS)


def draw_out_table(key, part):
    cols = jnp.arange(D, dtype=jnp.float32) / D
    jitter = jnp.exp(jax.random.uniform(jax.random.fold_in(key, 2), (D,), jnp.float32, -0.35, 0.35))
    rowscale = jnp.exp(jax.random.uniform(jax.random.fold_in(key, 3), (EXPERTS, 1), jnp.float32, 0.0, math.log(10.0)))
    base = jax.random.normal(jax.random.fold_in(key, 6), (EXPERTS, D), jnp.float32)
    colscale = 10.0 ** cols * jitter
    return (0.1 * base * rowscale * colscale[None, :]).astype(jnp.bfloat16)


def block_scale(key, extent, cuts, least, top_value):
    level, own = 1.0, jax.random.fold_in(key, 6)
    for dim, shards_of in cuts:
        steps = jnp.exp(jax.random.uniform(jax.random.fold_in(own, dim), (shards_of,), jnp.float32, least / len(cuts), top_value / len(cuts)))
        level = level * jnp.repeat(steps, extent[dim] // shards_of).reshape([-1 if axis == dim else 1 for axis in range(len(extent))])
    return level


def scatter_about(stream_key, extent, spread, most, cuts=(), kind=jnp.bfloat16):
    level = block_scale(stream_key, extent, cuts, -0.22, 0.18) if cuts else 1.0
    values = jax.random.normal(stream_key, extent, jnp.float32) * spread * level
    return jnp.minimum(jnp.maximum(values, -most), most).astype(kind)


def setup_inputs(seed: int = 0) -> dict:
    key_of = jax.random.split(jax.random.key(seed), 7)
    tokens = scatter_about(key_of[0], (TOKENS, D), 1.0, 6.0, ((0, 16), (1, 2)))
    experts = draw_experts(jax.random.fold_in(key_of[6], 71), 0)
    weights = jnp.clip(jnp.exp(math.log(1.0) - 2.9957323 * jax.random.uniform(key_of[2], (TOKENS, SLOTS), jnp.float32) ** block_scale(key_of[2], (TOKENS, SLOTS), ((0, 16),), -0.2, 0.2)), 0.05, 1.0)
    up_table = scatter_about(key_of[3], (EXPERTS, D), D ** -0.5, 0.125, ((0, 16), (1, 2)))
    out_table = draw_out_table(jax.random.fold_in(key_of[6], 71), 0)
    gain = jnp.clip(1.0 + 0.18 * jax.random.normal(key_of[5], (D,), jnp.float32), 0.1, 1.9)
    return {"tokens": tokens, "experts": experts, "weights": weights, "up_table": up_table, "out_table": out_table, "gain": gain}


def reference(tokens, experts, weights, up_table, out_table, gain):
    blocks = tokens.shape[0] // TOK_DEV
    tok_blocks = tokens.reshape(blocks, TOK_DEV, D)
    id_blocks = experts.reshape(blocks, TOK_DEV, SLOTS)
    wt_blocks = weights.reshape(blocks, TOK_DEV, SLOTS)
    gain_f = gain.astype(jnp.float32)

    def one_block(args):
        rows, ids, wts = args
        up_rows = up_table[ids].astype(jnp.float32)
        dot = jnp.einsum('tw,tkw->tk', rows.astype(jnp.float32), up_rows)
        act = jax.nn.gelu(dot)
        contrib = (act[:, :, None] * out_table[ids].astype(jnp.float32)).astype(jnp.bfloat16)
        mixed = jnp.einsum('tk,tkw->tw', wts.astype(jnp.float32), contrib.astype(jnp.float32))
        power = lax.optimization_barrier(jnp.mean(mixed * mixed, axis=1))
        return (mixed * lax.rsqrt(power + 1e-06)[:, None] * gain_f[None, :]).astype(jnp.bfloat16)
    normed = lax.map(one_block, (tok_blocks, id_blocks, wt_blocks))
    return normed.reshape(tokens.shape[0], D)
```

```python
import functools
import itertools

import jax
import jax.numpy as jnp
import numpy as np
from jax import lax
from jax.experimental import pallas as pl
from jax.experimental.pallas import tpu as pltpu
from jax.sharding import PartitionSpec as P

LANES = 128
MESH = pl.DeviceIdType.MESH
NT = (((1,), (1,)), ((), ()))
VMEM_LIMIT = 60 * 1024 * 1024


def ep_dims(mesh):
    n = mesh.shape["ep"]
    devices = np.moveaxis(mesh.devices, mesh.axis_names.index("ep"), 0).reshape(n, -1)[:, 0]
    coords = [getattr(d, "coords", None) for d in devices]
    if any(c is None for c in coords):
        return (n,)
    axes = []
    for a in range(len(coords[0])):
        values = [c[a] for c in coords]
        size = len(set(values))
        if size > 1:
            stride = next(i for i in range(n) if values[i] != values[0])
            axes.append((stride, size, [v - min(values) for v in values]))
    axes.sort(key=lambda t: -t[0])
    dims = tuple(size for _, size, _ in axes)
    if int(np.prod(dims)) != n:
        return (n,)
    for i in range(n):
        if any((i // stride) % size != values[i] for stride, size, values in axes):
            return (n,)
    return dims


def tree_plans(dims, rows):
    k = len(dims)
    if k == 3 and rows % 128 == 0:
        long, mid, last = sorted(range(3), key=lambda i: -dims[i])
        unit = rows // 8
        plans = [
            ((long, mid, last), 3 * unit),
            ((long, last, mid), 3 * unit),
            ((last, mid, long), unit),
            ((mid, last, long), unit),
        ]
    elif k == 2 and rows % 32 == 0:
        plans = [((0, 1), rows // 2), ((1, 0), rows // 2)]
    else:
        plans = [(tuple(range(k)), rows)]
    out, first = [], 0
    for order, count in plans:
        out.append((order, first, count))
        first += count
    return out


class Place:
    def __init__(self, dims):
        self.dims = dims
        self.strides = [int(np.prod(dims[i + 1 :])) for i in range(len(dims))]
        self.e = lax.axis_index("ep")
        self.tp = lax.axis_index("tp")
        self.at = [(self.e // st) % n for st, n in zip(self.strides, dims)]

    def near(self, dim, k):
        m, n = self.at[dim], self.dims[dim]
        if k == 0:
            return m
        if n == 2:
            return 1 - m
        below, above = m, n - 1 - m
        low = jnp.minimum(below, above)
        hop = (k + 1) // 2
        alternate = m + hop if k % 2 else m - hop
        far = jnp.where(below < above, m + (k - low), m - (k - low))
        return jnp.where(k <= 2 * low, alternate, far)

    def flat(self, coords):
        total = 0
        for c, st in zip(coords, self.strides):
            total = total + c * st
        return total

    def moved(self, dim, to):
        return self.e + (to - self.at[dim]) * self.strides[dim]


def tree_events(order, dims):
    events = []
    for j in range(len(order)):
        heads = [range(dims[order[i]]) for i in range(j)] + [range(1, dims[order[j]])]
        for ks in itertools.product(*heads):
            events.append((j, ks))
    return events


def event_block(place, order, j, ks):
    coords = list(place.at)
    for i in range(j + 1):
        coords[order[i]] = place.near(order[i], ks[i])
    return coords


def tree_neighbors(place, order, j, coords):
    out = []
    for l in range(max(j, 0), len(order)):
        dim = order[l]
        n, m = place.dims[dim], place.at[dim]
        if l == j:
            if n > 2:
                to = m + jnp.where(m > coords[dim], 1, -1)
                out.append((l, to, (to >= 0) & (to < n)))
        elif n == 2:
            out.append((l, 1 - m, None))
        else:
            out.append((l, m + 1, m + 1 < n))
            out.append((l, m - 1, m > 0))
    return out


def schedule(plans, dims):
    keyed = []
    for v, (order, _, count) in enumerate(plans):
        seen = {}
        for j, ks in tree_events(order, dims):
            dist = sum((k + 1) // 2 if dims[order[i]] > 2 else k for i, k in enumerate(ks))
            before = seen.get(j, 0)
            seen[j] = before + 1
            keyed.append(((dist + before) * 1.0 + 0.01 * j, v, j, ks))
    keyed.sort(key=lambda t: t[0])
    return [(v, j, ks) for _, v, j, ks in keyed]


def maybe(pred, fn):
    if pred is None:
        fn()
    else:
        pl.when(pred)(fn)


def route_kernel(n_ep, cap, rows_held, experts_ref, weights_ref, list_ref):
    slots, tok_rows = experts_ref.shape
    col = lax.broadcasted_iota(jnp.int32, (tok_rows, tok_rows), 1)
    row = lax.broadcasted_iota(jnp.int32, (tok_rows, tok_rows), 0)
    before = (row < col).astype(jnp.float32).astype(jnp.bfloat16)
    owners = lax.broadcasted_iota(jnp.int32, (n_ep, tok_rows), 0)
    places = lax.broadcasted_iota(jnp.int32, (cap, tok_rows), 0)
    token = lax.broadcasted_iota(jnp.int32, (1, tok_rows), 1)
    base = jnp.zeros((n_ep, 1), jnp.float32)
    total = jnp.zeros((6 * n_ep, cap), jnp.float32)
    for k in range(slots):
        e = experts_ref[k : k + 1, :]
        owner = e // rows_held
        mine = owner == owners
        ones = jnp.where(mine, 1.0, 0.0)
        ahead = jnp.dot(ones.astype(jnp.bfloat16), before, preferred_element_type=jnp.float32) + base
        base = base + jnp.sum(ones, axis=1, keepdims=True)
        rank = jnp.sum(jnp.where(mine, ahead, 0.0), axis=0, keepdims=True).astype(jnp.int32)
        at = jnp.where(rank == places, 1.0, 0.0).astype(jnp.bfloat16)
        word = token * rows_held + (e - owner * rows_held)
        w = weights_ref[k : k + 1, :]
        w0 = w.astype(jnp.bfloat16).astype(jnp.float32)
        w1 = (w - w0).astype(jnp.bfloat16).astype(jnp.float32)
        w2 = w - w0 - w1
        parts = [(word & 255), ((word >> 8) & 255), (word >> 16)]
        parts = [p.astype(jnp.float32) for p in parts] + [w0, w1, w2]
        lhs = jnp.concatenate([jnp.where(mine, p, 0.0) for p in parts], axis=0).astype(jnp.bfloat16)
        total = total + lax.dot_general(lhs, at, NT, preferred_element_type=jnp.float32)
    take = lambda i: total[i * n_ep : (i + 1) * n_ep, :]
    list_ref[:, 0, :] = take(0) + 256.0 * take(1) + 65536.0 * take(2)
    list_ref[:, 1, :] = take(3) + take(4) + take(5)


def route(experts_t, weights_t, n_ep, cap, rows_held):
    return pl.pallas_call(
        functools.partial(route_kernel, n_ep, cap, rows_held),
        out_shape=jax.ShapeDtypeStruct((n_ep, 2, cap), jnp.float32),
        compiler_params=pltpu.CompilerParams(vmem_limit_bytes=VMEM_LIMIT),
        name="route",
    )(experts_t, weights_t)


def count_sends(plans, dims):
    total = 0
    for order, _, _ in plans:
        for j, _ in [(-1, ())] + tree_events(order, dims):
            for l in range(max(j, 0), len(order)):
                big = dims[order[l]] > 2
                total += (1 if big else 0) if l == j else (2 if big else 1)
    return total


def gather_kernel(dims, plans, tok_ref, list_ref, all_ref, lists_ref, ssem, rsem, lssem, lrsem):
    place = Place(dims)
    n_ep = all_ref.shape[0]
    me = place.e
    barrier = pltpu.get_barrier_semaphore()
    for o in range(1, n_ep):
        pl.semaphore_signal(barrier, inc=1, device_id=((me + o) % n_ep, place.tp), device_id_type=MESH)
    pl.semaphore_wait(barrier, n_ep - 1)

    list_copies = []
    for o in range(1, n_ep):
        to = (me + o) % n_ep
        copy = pltpu.make_async_remote_copy(
            src_ref=list_ref.at[to],
            dst_ref=lists_ref.at[me],
            send_sem=lssem.at[o],
            recv_sem=lrsem.at[o],
            device_id=(to, place.tp),
            device_id_type=MESH,
        )
        copy.start()
        list_copies.append(copy)

    sends = []

    def forward(v, j, coords, src):
        order, first, count = plans[v]
        s = place.flat(coords)
        for l, to, pred in tree_neighbors(place, order, j, coords):
            copy = pltpu.make_async_remote_copy(
                src_ref=src,
                dst_ref=all_ref.at[s, pl.ds(first, count)],
                send_sem=ssem.at[len(sends)],
                recv_sem=rsem.at[v, s],
                device_id=(place.moved(order[l], to), place.tp),
                device_id_type=MESH,
            )
            maybe(pred, copy.start)
            sends.append((pred, copy))

    for v, (order, first, count) in enumerate(plans):
        forward(v, -1, place.at, tok_ref.at[pl.ds(first, count)])
    all_ref[me] = tok_ref[...]
    lists_ref[me] = list_ref[me]
    for v, j, ks in schedule(plans, dims):
        order, first, count = plans[v]
        coords = event_block(place, order, j, ks)
        s = place.flat(coords)
        block = all_ref.at[s, pl.ds(first, count)]
        pltpu.make_async_remote_copy(
            src_ref=block,
            dst_ref=block,
            send_sem=ssem.at[0],
            recv_sem=rsem.at[v, s],
            device_id=(me, place.tp),
            device_id_type=MESH,
        ).wait_recv()
        forward(v, j, coords, block)
    for copy in list_copies:
        copy.wait()
    for pred, copy in sends:
        maybe(pred, copy.wait_send)


def gather_tokens(tokens, lists, dims, plans):
    n_ep = int(np.prod(dims))
    vmem = pl.BlockSpec(memory_space=pltpu.VMEM)
    return pl.pallas_call(
        functools.partial(gather_kernel, dims, plans),
        out_shape=(
            jax.ShapeDtypeStruct((n_ep,) + tokens.shape, tokens.dtype),
            jax.ShapeDtypeStruct(lists.shape, lists.dtype),
        ),
        in_specs=[vmem, vmem],
        out_specs=(vmem, vmem),
        scratch_shapes=[
            pltpu.SemaphoreType.DMA((count_sends(plans, dims),)),
            pltpu.SemaphoreType.DMA((len(plans), n_ep)),
            pltpu.SemaphoreType.DMA((n_ep,)),
            pltpu.SemaphoreType.DMA((n_ep,)),
        ],
        compiler_params=pltpu.CompilerParams(
            collective_id=0, has_side_effects=True, vmem_limit_bytes=VMEM_LIMIT
        ),
        name="gather_tokens",
    )(tokens, lists)


def load_table(table_ref, flat, stage, sem):
    rows, width = table_ref.shape
    sub = width // LANES
    step = stage.shape[1]
    chunks = rows // step

    def copy(i, slot):
        return pltpu.make_async_copy(table_ref.at[pl.ds(i * step, step)], stage.at[slot], sem.at[slot])

    copy(0, 0).start()
    for i in range(chunks):
        slot = i % 2
        if i + 1 < chunks:
            copy(i + 1, 1 - slot).start()
        copy(i, slot).wait()

        def spread(g, carry):
            r = pl.multiple_of(g * 16, 16)
            for c in range(sub):
                x = stage[slot, pl.ds(r, 16), c * LANES : (c + 1) * LANES].astype(jnp.float32)
                for h in range(2):
                    first = (i * step + r + 8 * h) * sub + c
                    flat[pl.ds(first, 8, stride=sub), :] = x[8 * h : 8 * h + 8, :]
            return carry

        lax.fori_loop(0, step // 16, spread, 0)


def take_rows(row_ref, first, cap, sub, flat, picked, packed):
    unroll = 32

    def some(g, carry):
        for u in range(unroll):
            r = g * unroll + u
            at = pl.multiple_of(row_ref[first + r], sub)
            picked[pl.ds(pl.multiple_of(r * sub, sub), sub), :] = flat[pl.ds(at, sub), :]
        return carry

    lax.fori_loop(0, cap // unroll, some, 0)
    for c in range(sub):
        lines = picked[pl.ds(c, cap, stride=sub), :] if sub > 1 else picked[...]
        packed[:, c * LANES : (c + 1) * LANES] = lines.astype(jnp.bfloat16)


def hits(list_ref, s, tok_rows, rows_held):
    cap = list_ref.shape[2]
    word = list_ref[s, 0:1, :].astype(jnp.int32)
    return (word // rows_held) == lax.broadcasted_iota(jnp.int32, (tok_rows, cap), 0)


def dots_kernel(row_ref, list_ref, tok_ref, table_ref, dot_ref, stage, flat, picked, packed, sem):
    n_ep, tok_rows, width = tok_ref.shape
    cap = list_ref.shape[2]
    sub = width // LANES
    load_table(table_ref, flat, stage, sem)

    def source(s, carry):
        take_rows(row_ref, s * cap, cap, sub, flat, picked, packed)
        full = lax.dot_general(tok_ref[s], packed[...], NT, preferred_element_type=jnp.float32)
        hit = hits(list_ref, s, tok_rows, table_ref.shape[0])
        dot_ref[s] = jnp.sum(jnp.where(hit, full, 0.0), axis=0, keepdims=True)
        return carry

    lax.fori_loop(0, n_ep, source, 0)


def mix_kernel(row_ref, list_ref, coef_ref, table_ref, mix_ref, stage, flat, picked, packed, sem):
    n_ep, tok_rows, width = mix_ref.shape
    cap = list_ref.shape[2]
    sub = width // LANES
    load_table(table_ref, flat, stage, sem)

    def source(s, carry):
        take_rows(row_ref, s * cap, cap, sub, flat, picked, packed)
        hit = hits(list_ref, s, tok_rows, table_ref.shape[0])
        coef = coef_ref[s]
        high = coef.astype(jnp.bfloat16).astype(jnp.float32)
        low = coef - high
        rows = packed[...]
        mixed = jnp.dot(jnp.where(hit, high, 0.0).astype(jnp.bfloat16), rows, preferred_element_type=jnp.float32)
        mixed += jnp.dot(jnp.where(hit, low, 0.0).astype(jnp.bfloat16), rows, preferred_element_type=jnp.float32)
        mix_ref[s] = mixed.astype(jnp.bfloat16)
        return carry

    lax.fori_loop(0, n_ep, source, 0)


def table_scratch(rows, width, cap):
    sub = width // LANES
    step = min(rows, 512)
    return [
        pltpu.VMEM((2, step, width), jnp.bfloat16),
        pltpu.VMEM((rows * sub, LANES), jnp.float32),
        pltpu.VMEM((cap * sub, LANES), jnp.float32),
        pltpu.VMEM((cap, width), jnp.bfloat16),
        pltpu.SemaphoreType.DMA((2,)),
    ]


def row_call(kernel, out, row_at, lists, middle, table, name):
    cap = lists.shape[2]
    vmem = pl.BlockSpec(memory_space=pltpu.VMEM)
    return pl.pallas_call(
        kernel,
        in_specs=[
            pl.BlockSpec(memory_space=pltpu.SMEM),
            vmem,
            vmem,
            pl.BlockSpec(memory_space=pl.ANY),
        ],
        out_specs=vmem,
        scratch_shapes=table_scratch(*table.shape, cap),
        out_shape=out,
        compiler_params=pltpu.CompilerParams(vmem_limit_bytes=VMEM_LIMIT),
        name=name,
    )(row_at, lists, middle, table)


def stage_layout(order, dims):
    bases, base = [], 0
    for j, dim in enumerate(order):
        bases.append(base)
        inner = int(np.prod([dims[order[i]] for i in range(j)]))
        base += (2 * dims[dim] if dims[dim] > 2 else 1) * inner
    return bases, base


def stage_slot(dims, order, bases, j, side, coords):
    n = dims[order[j]]
    inner, width = 0, 1
    for i in reversed(range(j)):
        inner = inner + coords[order[i]] * width
        width *= dims[order[i]]
    outer = (side * n + coords[order[j]]) if n > 2 else 0
    return bases[j] + outer * width + inner


def scatter_kernel(dims, plans, given_ref, out_ref, part_ref, *scratch):
    held = scratch[: len(plans)]
    rsems = scratch[len(plans) : 2 * len(plans)]
    ssem = scratch[-1]
    place = Place(dims)
    me = place.e
    barrier = pltpu.get_barrier_semaphore()
    around = []
    for dim, n in enumerate(dims):
        m = place.at[dim]
        if n == 2:
            around.append((place.moved(dim, 1 - m), None))
        else:
            around.append((place.moved(dim, m + 1), m + 1 < n))
            around.append((place.moved(dim, m - 1), m > 0))
    for to, pred in around:
        def greet(to=to):
            pl.semaphore_signal(barrier, inc=1, device_id=(to, place.tp), device_id_type=MESH)
        maybe(pred, greet)
    met = sum(1 if pred is None else jnp.where(pred, 1, 0) for _, pred in around)
    pl.semaphore_wait(barrier, met)

    load = pltpu.make_async_copy(given_ref, part_ref, scratch[-2])
    load.start()
    load.wait()
    layouts = [stage_layout(order, dims)[0] for order, _, _ in plans]
    sends = []

    def incoming(v, j, coords):
        order = plans[v][0]
        out = []
        for l, frm, pred in tree_neighbors(place, order, j, coords):
            dim = order[l]
            side = jnp.where(frm > place.at[dim], 1, 0)
            out.append((stage_slot(dims, order, layouts[v], l, side, coords), pred))
        out.sort(key=lambda t: t[1] is not None)
        return out

    def await_slot(v, slot):
        ref = held[v].at[slot]
        pltpu.make_async_remote_copy(
            src_ref=ref, dst_ref=ref, send_sem=ssem.at[0], recv_sem=rsems[v].at[slot],
            device_id=(me, place.tp), device_id_type=MESH,
        ).wait_recv()

    def add(v, d, slots, final):
        _, first, count = plans[v]
        unit = 16 if count % 16 == 0 else count

        def some(i, carry):
            r = pl.multiple_of(i * unit, unit)
            rows = pl.ds(first + r, unit)
            x = part_ref[d, rows, :].astype(jnp.float32)
            for slot in slots:
                x = x + held[v][slot, pl.ds(r, unit), :].astype(jnp.float32)
            if final:
                out_ref[rows, :] = x
            else:
                part_ref[d, rows, :] = x.astype(jnp.bfloat16)
            return carry

        lax.fori_loop(0, count // unit, some, 0)

    def collect(v, d, inc, final):
        sure = [slot for slot, pred in inc if pred is None]
        unsure = [(slot, pred) for slot, pred in inc if pred is not None]
        for slot in sure:
            await_slot(v, slot)
        for slot, pred in unsure:
            maybe(pred, functools.partial(await_slot, v, slot))
        if not unsure:
            if sure or final:
                add(v, d, sure, final)
            return
        for picks in itertools.product((True, False), repeat=len(unsure)):
            cond = None
            for (_, pred), yes in zip(unsure, picks):
                term = pred if yes else jnp.logical_not(pred)
                cond = term if cond is None else cond & term
            slots = sure + [slot for (slot, _), yes in zip(unsure, picks) if yes]
            if slots or final:
                maybe(cond, functools.partial(add, v, d, slots, final))

    for v, j, ks in reversed(schedule(plans, dims)):
        order, first, count = plans[v]
        coords = event_block(place, order, j, ks)
        d = place.flat(coords)
        collect(v, d, incoming(v, j, coords), False)
        dim = order[j]
        m = place.at[dim]
        to = 1 - m if dims[dim] == 2 else m + jnp.where(coords[dim] > m, 1, -1)
        side = jnp.where(m > to, 1, 0)
        slot = stage_slot(dims, order, layouts[v], j, side, coords)
        copy = pltpu.make_async_remote_copy(
            src_ref=part_ref.at[d, pl.ds(first, count)],
            dst_ref=held[v].at[slot],
            send_sem=ssem.at[len(sends)],
            recv_sem=rsems[v].at[slot],
            device_id=(place.moved(dim, to), place.tp),
            device_id_type=MESH,
        )
        copy.start()
        sends.append(copy)
    for v, (order, first, count) in enumerate(plans):
        collect(v, me, incoming(v, -1, place.at), True)
    for copy in sends:
        copy.wait_send()


def scatter_sum(part, dims, plans):
    n_ep, tok_rows, width = part.shape
    counts = [(stage_layout(order, dims)[1], count) for order, _, count in plans]
    vmem = pl.BlockSpec(memory_space=pltpu.VMEM)
    return pl.pallas_call(
        functools.partial(scatter_kernel, dims, plans),
        out_shape=jax.ShapeDtypeStruct((tok_rows, width), jnp.float32),
        in_specs=[pl.BlockSpec(memory_space=pl.ANY)],
        out_specs=vmem,
        scratch_shapes=[pltpu.VMEM(part.shape, jnp.bfloat16)]
        + [pltpu.VMEM((slots, count, width), jnp.bfloat16) for slots, count in counts]
        + [pltpu.SemaphoreType.DMA((slots,)) for slots, _ in counts]
        + [pltpu.SemaphoreType.DMA, pltpu.SemaphoreType.DMA((len(schedule(plans, dims)),))],
        compiler_params=pltpu.CompilerParams(
            collective_id=1, has_side_effects=True, vmem_limit_bytes=VMEM_LIMIT
        ),
        name="scatter_sum",
    )(part)


def body(dims, tokens, experts, weights, up_table, out_table, gain):
    n_ep = lax.axis_size("ep")
    tok_rows, width = tokens.shape
    slots = experts.shape[1]
    rows_held = up_table.shape[0]
    sub = width // LANES
    cap = 2 * tok_rows * slots // n_ep
    plans = tree_plans(dims, tok_rows)
    lists = route(experts.T, weights.T, n_ep, cap, rows_held)
    tok_all, lists_all = gather_tokens(tokens, lists, dims, plans)
    row_at = ((lists_all[:, 0, :].astype(jnp.int32) % rows_held) * sub).reshape(-1)
    dot_shape = jax.ShapeDtypeStruct((n_ep, 1, cap), jnp.float32)
    partial_dot = row_call(dots_kernel, dot_shape, row_at, lists_all, tok_all, up_table, "request_dots")
    dot = lax.psum(partial_dot, "tp")
    coef = lists_all[:, 1:2, :] * jax.nn.gelu(dot)
    part_shape = jax.ShapeDtypeStruct((n_ep, tok_rows, width), jnp.bfloat16)
    part = row_call(mix_kernel, part_shape, row_at, lists_all, coef, out_table, "mix_rows")
    mixed = scatter_sum(part, dims, plans)
    square = lax.psum(jnp.sum(mixed * mixed, axis=1), "tp")
    scale = lax.rsqrt(square / (width * lax.axis_size("tp")) + 1e-06)
    return (mixed * scale[:, None] * gain[None, :]).astype(jnp.bfloat16)


def solution(mesh):
    placed = (P("ep", "tp"), P("ep", None), P("ep", None), P("ep", "tp"), P("ep", "tp"), P("tp"))
    return jax.shard_map(
        functools.partial(body, ep_dims(mesh)), mesh=mesh, in_specs=placed, out_specs=P("ep", "tp"), check_vma=False
    )
```

```python
import functools
import itertools

import jax
import jax.numpy as jnp
import numpy as np
from jax import lax
from jax.experimental import pallas as pl
from jax.experimental.pallas import tpu as pltpu
from jax.sharding import PartitionSpec as P

LANES = 128
MESH = pl.DeviceIdType.MESH
NT = (((1,), (1,)), ((), ()))
VMEM_LIMIT = 63 * 1024 * 1024
PITCH = 9
DEPTH = 8
SCATTER_ORDER = ()
GATHER_ORDER = (
    0, 15, 1, 31, 30, 46, 45, 18, 48, 3, 49, 19, 16, 5, 36, 7, 11, 37, 51, 54, 47, 4, 32, 52, 33, 55,
    50, 39, 34, 20, 2, 17, 58, 42, 22, 25, 40, 57, 43, 6, 35, 41, 9, 12, 24, 53, 28, 21, 13, 26, 10, 44,
    59, 56, 8, 38, 27, 14, 23, 29,
)


def ep_dims(mesh):
    n = mesh.shape["ep"]
    devices = np.moveaxis(mesh.devices, mesh.axis_names.index("ep"), 0).reshape(n, -1)[:, 0]
    coords = [getattr(d, "coords", None) for d in devices]
    if any(c is None for c in coords):
        return (n,)
    axes = []
    for a in range(len(coords[0])):
        values = [c[a] for c in coords]
        size = len(set(values))
        if size > 1:
            stride = next(i for i in range(n) if values[i] != values[0])
            axes.append((stride, size, [v - min(values) for v in values]))
    axes.sort(key=lambda t: -t[0])
    dims = tuple(size for _, size, _ in axes)
    if int(np.prod(dims)) != n:
        return (n,)
    for i in range(n):
        if any((i // stride) % size != values[i] for stride, size, values in axes):
            return (n,)
    return dims


def tree_plans(dims, rows):
    k = len(dims)
    if k == 3 and rows % 128 == 0:
        long, mid, last = sorted(range(3), key=lambda i: -dims[i])
        unit = rows // 8
        plans = [
            ((long, mid, last), 3 * unit),
            ((long, last, mid), 3 * unit),
            ((last, mid, long), unit),
            ((mid, last, long), unit),
        ]
    elif k == 2 and rows % 32 == 0:
        plans = [((0, 1), rows // 2), ((1, 0), rows // 2)]
    else:
        plans = [(tuple(range(k)), rows)]
    out, first = [], 0
    for order, count in plans:
        out.append((order, first, count))
        first += count
    return out


class Place:
    def __init__(self, dims):
        self.dims = dims
        self.strides = [int(np.prod(dims[i + 1 :])) for i in range(len(dims))]
        self.e = lax.axis_index("ep")
        self.tp = lax.axis_index("tp")
        self.at = [(self.e // st) % n for st, n in zip(self.strides, dims)]

    def near(self, dim, k):
        m, n = self.at[dim], self.dims[dim]
        if k == 0:
            return m
        if n == 2:
            return 1 - m
        below, above = m, n - 1 - m
        low = jnp.minimum(below, above)
        hop = (k + 1) // 2
        alternate = m + hop if k % 2 else m - hop
        far = jnp.where(below < above, m + (k - low), m - (k - low))
        return jnp.where(k <= 2 * low, alternate, far)

    def flat(self, coords):
        total = 0
        for c, st in zip(coords, self.strides):
            total = total + c * st
        return total

    def moved(self, dim, to):
        return self.e + (to - self.at[dim]) * self.strides[dim]


def tree_events(order, dims):
    events = []
    for j in range(len(order)):
        heads = [range(dims[order[i]]) for i in range(j)] + [range(1, dims[order[j]])]
        for ks in itertools.product(*heads):
            events.append((j, ks))
    return events


def event_block(place, order, j, ks):
    coords = list(place.at)
    for i in range(j + 1):
        coords[order[i]] = place.near(order[i], ks[i])
    return coords


def tree_neighbors(place, order, j, coords):
    out = []
    for l in range(max(j, 0), len(order)):
        dim = order[l]
        n, m = place.dims[dim], place.at[dim]
        if l == j:
            if n > 2:
                to = m + jnp.where(m > coords[dim], 1, -1)
                out.append((l, to, (to >= 0) & (to < n)))
        elif n == 2:
            out.append((l, 1 - m, None))
        else:
            out.append((l, m + 1, m + 1 < n))
            out.append((l, m - 1, m > 0))
    return out


def schedule(plans, dims, table):
    keyed = []
    for v, (order, _, count) in enumerate(plans):
        seen = {}
        for j, ks in tree_events(order, dims):
            dist = sum((k + 1) // 2 if dims[order[i]] > 2 else k for i, k in enumerate(ks))
            before = seen.get(j, 0)
            seen[j] = before + 1
            keyed.append(((dist + before) * 1.0 + 0.01 * j, v, j, ks))
    events = [(v, j, ks) for _, v, j, ks in keyed]
    if len(events) == len(table):
        return [events[i] for i in table]
    keyed.sort(key=lambda t: t[0])
    return [(v, j, ks) for _, v, j, ks in keyed]


def relative(plans, v, ks):
    order = plans[v][0]
    ranks = [0] * len(order)
    for i, k in enumerate(ks):
        ranks[order[i]] = k
    return tuple(ranks)


def block_of(place, ranks):
    return place.flat([place.near(dim, k) for dim, k in enumerate(ranks)])


def maybe(pred, fn):
    if pred is None:
        fn()
    else:
        pl.when(pred)(fn)


def count_sends(plans, dims):
    total = 0
    for order, _, _ in plans:
        for j, _ in [(-1, ())] + tree_events(order, dims):
            for l in range(max(j, 0), len(order)):
                big = dims[order[l]] > 2
                total += (1 if big else 0) if l == j else (2 if big else 1)
    return total


def route_kernel(n_ep, cap, rows_held, sub, experts_ref, weights_ref, word_ref, weight_ref):
    slots, tok_rows = experts_ref.shape
    col = lax.broadcasted_iota(jnp.int32, (tok_rows, tok_rows), 1)
    row = lax.broadcasted_iota(jnp.int32, (tok_rows, tok_rows), 0)
    before = (row < col).astype(jnp.float32).astype(jnp.bfloat16)
    owners = lax.broadcasted_iota(jnp.int32, (n_ep, tok_rows), 0)
    places = lax.broadcasted_iota(jnp.int32, (cap, tok_rows), 0)
    token = lax.broadcasted_iota(jnp.int32, (1, tok_rows), 1)
    base = jnp.zeros((n_ep, 1), jnp.float32)
    total = jnp.zeros((6 * n_ep, cap), jnp.float32)
    for k in range(slots):
        e = experts_ref[k : k + 1, :]
        owner = e // rows_held
        mine = owner == owners
        ones = jnp.where(mine, 1.0, 0.0)
        ahead = jnp.dot(ones.astype(jnp.bfloat16), before, preferred_element_type=jnp.float32) + base
        base = base + jnp.sum(ones, axis=1, keepdims=True)
        rank = jnp.sum(jnp.where(mine, ahead, 0.0), axis=0, keepdims=True).astype(jnp.int32)
        at = jnp.where(rank == places, 1.0, 0.0).astype(jnp.bfloat16)
        word = token * rows_held + (e - owner * rows_held)
        w = weights_ref[k : k + 1, :]
        w0 = w.astype(jnp.bfloat16).astype(jnp.float32)
        w1 = (w - w0).astype(jnp.bfloat16).astype(jnp.float32)
        w2 = w - w0 - w1
        parts = [(word & 255), ((word >> 8) & 255), (word >> 16)]
        parts = [p.astype(jnp.float32) for p in parts] + [w0, w1, w2]
        lhs = jnp.concatenate([jnp.where(mine, p, 0.0) for p in parts], axis=0).astype(jnp.bfloat16)
        total = total + lax.dot_general(lhs, at, NT, preferred_element_type=jnp.float32)
    take = lambda i: total[i * n_ep : (i + 1) * n_ep, :]
    word = (take(0) + 256.0 * take(1) + 65536.0 * take(2)).astype(jnp.int32)
    token = word // rows_held
    row = word - token * rows_held
    line = (row // 8) * (sub * PITCH - 8) + row
    word_ref[:, 0, :] = token * lines_of(rows_held, sub) + line
    weight_ref[:, 0, :] = take(3) + take(4) + take(5)


def lines_of(rows_held, sub):
    return rows_held // 8 * sub * PITCH


def route(experts_t, weights_t, n_ep, cap, rows_held, sub):
    lists = (n_ep, 1, cap)
    return pl.pallas_call(
        functools.partial(route_kernel, n_ep, cap, rows_held, sub),
        out_shape=(jax.ShapeDtypeStruct(lists, jnp.int32), jax.ShapeDtypeStruct(lists, jnp.float32)),
        name="route",
    )(experts_t, weights_t)


def table_piece(table_ref, flat, stage, sem, i, slot):
    step, width = stage.shape[1:]
    sub = width // LANES
    copy = pltpu.make_async_copy(table_ref.at[pl.ds(i * step, step)], stage.at[slot], sem.at[slot])

    def rest():
        copy.wait()

        def spread(g, carry):
            r = pl.multiple_of(g * 16, 16)
            for c in range(sub):
                x = stage[slot, pl.ds(r, 16), c * LANES : (c + 1) * LANES].astype(jnp.float32)
                for h in range(2):
                    first = ((i * (step // 8) + g * 2 + h) * sub + c) * PITCH
                    flat[pl.ds(first, 8), :] = x[8 * h : 8 * h + 8, :]
            return carry

        lax.fori_loop(0, step // 16, spread, 0)

    return copy.start, rest


def take_rows(row_ref, s, sub, flat, picked, put):
    cap = row_ref.shape[1]
    unroll = 32
    gap = sub + 1 if sub > 1 else 1

    def some(g, carry):
        taken = []
        for u in range(unroll):
            at = row_ref[s, g * unroll + u]
            taken.append(flat[pl.ds(at, sub, stride=PITCH), :] if sub > 1 else flat[pl.ds(at, 1), :])
        for u in range(unroll):
            picked[pl.ds((g * unroll + u) * gap, sub), :] = taken[u]
        return carry

    lax.fori_loop(0, cap // unroll, some, 0)
    for c in range(sub):
        lines = picked[pl.ds(c, cap, stride=gap), :] if sub > 1 else picked[...]
        put(c, lines.astype(jnp.bfloat16))


def collect_kernel(
    dims, plans, n_tp, my_word, my_weight, tok_ref, up_ref, out_ref,
    coef_ref, word_ref, rows_ref,
    all_ref, weight_ref, row_held, row_ref, stage, flat, picked, packed, held, dots, others,
    ssem, rsem, wssem, wrsem, ossem, orsem, stage_sem, put_sem, row_sem,
):
    place = Place(dims)
    me = place.e
    n_ep, tok_rows, width = all_ref.shape
    cap = coef_ref.shape[2]
    rows_held = up_ref.shape[0]
    sub = width // LANES
    lines = lines_of(rows_held, sub)
    pieces = rows_held // stage.shape[1]
    depth = min(stage.shape[0], pieces)
    loads = [
        table_piece(table, flat, stage, stage_sem, i, i % depth) for table in (out_ref, up_ref) for i in range(pieces)
    ]
    for i in range(depth):
        loads[i][0]()

    barrier = pltpu.get_barrier_semaphore()
    for o in range(1, n_ep):
        pl.semaphore_signal(barrier, inc=1, device_id=((me + o) % n_ep, place.tp), device_id_type=MESH)
    for o in range(1, n_tp):
        pl.semaphore_signal(barrier, inc=1, device_id=(me, (place.tp + o) % n_tp), device_id_type=MESH)
    pl.semaphore_wait(barrier, n_ep + n_tp - 2)

    sends = []

    def forward(v, j, coords, src):
        order, first, count = plans[v]
        s = place.flat(coords)
        for l, to, pred in tree_neighbors(place, order, j, coords):
            copy = pltpu.make_async_remote_copy(
                src_ref=src,
                dst_ref=all_ref.at[s, pl.ds(first, count)],
                send_sem=ssem.at[len(sends)],
                recv_sem=rsem.at[v, s],
                device_id=(place.moved(order[l], to), place.tp),
                device_id_type=MESH,
            )
            maybe(pred, copy.start)
            sends.append((pred, copy))

    list_copies = []
    for o in range(1, n_ep):
        to = (me + o) % n_ep
        for i, (src, dst) in enumerate(((my_word, word_ref), (my_weight, weight_ref))):
            copy = pltpu.make_async_remote_copy(
                src_ref=src.at[to],
                dst_ref=dst.at[me],
                send_sem=wssem.at[i, o],
                recv_sem=wrsem.at[i, o],
                device_id=(to, place.tp),
                device_id_type=MESH,
            )
            copy.start()
            list_copies.append(copy)
    for v, (order, first, count) in enumerate(plans):
        forward(v, -1, place.at, tok_ref.at[pl.ds(first, count)])
    word_ref[me] = my_word[me]
    weight_ref[me] = my_weight[me]

    def load(i):
        loads[i][1]()
        if i + depth < len(loads):
            loads[i + depth][0]()

    def lists():
        for copy in list_copies:
            copy.wait_recv()
        for s in range(n_ep):
            word = word_ref[s]
            row_held[s : s + 1, :] = word - (word // lines) * lines
        copy = pltpu.make_async_copy(row_held, row_ref, row_sem)
        copy.start()
        copy.wait()

    def put_copy(s):
        return pltpu.make_async_copy(packed.at[s % 2], rows_ref.at[s], put_sem.at[s % 2])

    def out_rows(s):
        if s >= 2:
            put_copy(s - 2).wait()

        def put(c, lines):
            packed[s % 2, :, c * LANES : (c + 1) * LANES] = lines

        take_rows(row_ref, s, sub, flat, picked, put)
        put_copy(s).start()

    def up_rows(s):
        def put(c, lines):
            held[s, :, c * LANES : (c + 1) * LANES] = lines

        take_rows(row_ref, s, sub, flat, picked, put)

    def dot_of(ranks):
        s = block_of(place, ranks)
        tok = tok_ref[...] if not any(ranks) else all_ref[s]
        full = lax.dot_general(tok, held[s], NT, preferred_element_type=jnp.float32)
        hit = (word_ref[s] // lines) == lax.broadcasted_iota(jnp.int32, (tok_rows, cap), 0)
        dots[s] = jnp.sum(jnp.where(hit, full, 0.0), axis=0, keepdims=True)

    events = schedule(plans, dims, GATHER_ORDER)
    last = {}
    for i, (v, j, ks) in enumerate(events):
        last[relative(plans, v, ks)] = i
    work = [(0.3, functools.partial(load, i)) for i in range(pieces)] + [(0.5, lists)]
    work += [(0.8, functools.partial(out_rows, s)) for s in range(n_ep)]
    work += [(0.3, functools.partial(load, pieces + i)) for i in range(pieces)]
    work += [(0.8, functools.partial(up_rows, s)) for s in range(n_ep)]
    ready = [(0,) * len(dims)]
    clock, per_event = 3.0, 62.0 / len(events)
    for i, (v, j, ks) in enumerate(events):
        due = 4.0 + per_event * i
        while clock < due and (work or ready):
            if work:
                cost, fn = work.pop(0)
                fn()
                clock += cost
            else:
                dot_of(ready.pop(0))
                clock += 0.5
        clock = max(clock, due)
        order, first, count = plans[v]
        coords = event_block(place, order, j, ks)
        s = place.flat(coords)
        block = all_ref.at[s, pl.ds(first, count)]
        pltpu.make_async_remote_copy(
            src_ref=block, dst_ref=block, send_sem=ssem.at[0], recv_sem=rsem.at[v, s],
            device_id=(me, place.tp), device_id_type=MESH,
        ).wait_recv()
        forward(v, j, coords, block)
        ranks = relative(plans, v, ks)
        if last[ranks] == i:
            ready.append(ranks)
    for _, fn in work:
        fn()
    for ranks in ready:
        dot_of(ranks)

    shares = []
    for o in range(1, n_tp):
        copy = pltpu.make_async_remote_copy(
            src_ref=dots,
            dst_ref=others.at[o],
            send_sem=ossem.at[o],
            recv_sem=orsem.at[o],
            device_id=(me, (place.tp + o) % n_tp),
            device_id_type=MESH,
        )
        copy.start()
        shares.append(copy)
    for copy in shares:
        copy.wait_recv()

    def finish(s, carry):
        dot = dots[s]
        for o in range(1, n_tp):
            dot = dot + others[o, s]
        coef_ref[s] = weight_ref[s] * jax.nn.gelu(dot)
        return carry

    lax.fori_loop(0, n_ep, finish, 0)
    for copy in shares + list_copies:
        copy.wait_send()
    for s in range(max(0, n_ep - 2), n_ep):
        put_copy(s).wait()
    for pred, copy in sends:
        maybe(pred, copy.wait_send)


def collect(words, weights, tokens, up_table, out_table, dims, plans, n_tp, cap):
    n_ep = int(np.prod(dims))
    tok_rows, width = tokens.shape
    rows_held = up_table.shape[0]
    sub = width // LANES
    vmem = pl.BlockSpec(memory_space=pltpu.VMEM)
    hbm = pl.BlockSpec(memory_space=pl.ANY)
    lists = (n_ep, 1, cap)
    return pl.pallas_call(
        functools.partial(collect_kernel, dims, plans, n_tp),
        out_shape=(
            jax.ShapeDtypeStruct(lists, jnp.float32),
            jax.ShapeDtypeStruct(lists, jnp.int32),
            jax.ShapeDtypeStruct((n_ep, cap, width), jnp.bfloat16),
        ),
        in_specs=[vmem, vmem, vmem, hbm, hbm],
        out_specs=(vmem, vmem, hbm),
        scratch_shapes=[
            pltpu.VMEM((n_ep, tok_rows, width), jnp.bfloat16),
            pltpu.VMEM(lists, jnp.float32),
            pltpu.VMEM((n_ep, cap), jnp.int32),
            pltpu.SMEM((n_ep, cap), jnp.int32),
            pltpu.VMEM((DEPTH, min(rows_held, 256), width), jnp.bfloat16),
            pltpu.VMEM((lines_of(rows_held, sub), LANES), jnp.float32),
            pltpu.VMEM((cap * (sub + 1 if sub > 1 else 1), LANES), jnp.float32),
            pltpu.VMEM((2, cap, width), jnp.bfloat16),
            pltpu.VMEM((n_ep, cap, width), jnp.bfloat16),
            pltpu.VMEM(lists, jnp.float32),
            pltpu.VMEM((n_tp,) + lists, jnp.float32),
            pltpu.SemaphoreType.DMA((count_sends(plans, dims),)),
            pltpu.SemaphoreType.DMA((len(plans), n_ep)),
            pltpu.SemaphoreType.DMA((2, n_ep)),
            pltpu.SemaphoreType.DMA((2, n_ep)),
            pltpu.SemaphoreType.DMA((n_tp,)),
            pltpu.SemaphoreType.DMA((n_tp,)),
            pltpu.SemaphoreType.DMA((DEPTH,)),
            pltpu.SemaphoreType.DMA((2,)),
            pltpu.SemaphoreType.DMA,
        ],
        compiler_params=pltpu.CompilerParams(
            collective_id=0, has_side_effects=True, vmem_limit_bytes=VMEM_LIMIT
        ),
        name="collect",
    )(words, weights, tokens, up_table, out_table)


def stage_layout(order, dims):
    bases, base = [], 0
    for j, dim in enumerate(order):
        bases.append(base)
        inner = int(np.prod([dims[order[i]] for i in range(j)]))
        base += (2 * dims[dim] if dims[dim] > 2 else 1) * inner
    return bases, base


def stage_slot(dims, order, bases, j, side, coords):
    n = dims[order[j]]
    inner, width = 0, 1
    for i in reversed(range(j)):
        inner = inner + coords[order[i]] * width
        width *= dims[order[i]]
    outer = (side * n + coords[order[j]]) if n > 2 else 0
    return bases[j] + outer * width + inner


def scatter_kernel(dims, plans, n_tp, lines, coef_ref, word_ref, gain_ref, rows_ref, out_ref, part_ref, mixed, squares, others, rows, *scratch):
    held = scratch[: len(plans)]
    rsems = scratch[len(plans) : 2 * len(plans)]
    row_sem, ossem, orsem, ssem = scratch[-4:]
    place = Place(dims)
    me = place.e
    n_ep, tok_rows, width = part_ref.shape
    cap = coef_ref.shape[2]
    events = list(reversed(schedule(plans, dims, SCATTER_ORDER)))
    needed = []
    for v, j, ks in events:
        ranks = relative(plans, v, ks)
        if ranks not in needed:
            needed.append(ranks)
    needed.append((0,) * len(dims))
    depth = rows.shape[0]

    def fetch(i):
        return pltpu.make_async_copy(rows_ref.at[block_of(place, needed[i])], rows.at[i % depth], row_sem.at[i % depth])

    for i in range(min(depth, n_ep)):
        fetch(i).start()
    barrier = pltpu.get_barrier_semaphore()
    around = []
    for dim, n in enumerate(dims):
        m = place.at[dim]
        if n == 2:
            around.append((place.moved(dim, 1 - m), None))
        else:
            around.append((place.moved(dim, m + 1), m + 1 < n))
            around.append((place.moved(dim, m - 1), m > 0))
    for to, pred in around:
        def greet(to=to):
            pl.semaphore_signal(barrier, inc=1, device_id=(to, place.tp), device_id_type=MESH)
        maybe(pred, greet)
    for o in range(1, n_tp):
        pl.semaphore_signal(barrier, inc=1, device_id=(me, (place.tp + o) % n_tp), device_id_type=MESH)
    met = sum(1 if pred is None else jnp.where(pred, 1, 0) for _, pred in around)
    pl.semaphore_wait(barrier, met + n_tp - 1)

    layouts = [stage_layout(order, dims)[0] for order, _, _ in plans]
    sends = []

    def mix(i):
        d = block_of(place, needed[i])
        fetch(i).wait()
        hit = (word_ref[d] // lines) == lax.broadcasted_iota(jnp.int32, (tok_rows, cap), 0)
        coef = coef_ref[d]
        high = coef.astype(jnp.bfloat16).astype(jnp.float32)
        low = coef - high
        table_rows = rows[i % depth]
        total = jnp.dot(jnp.where(hit, high, 0.0).astype(jnp.bfloat16), table_rows, preferred_element_type=jnp.float32)
        total += jnp.dot(jnp.where(hit, low, 0.0).astype(jnp.bfloat16), table_rows, preferred_element_type=jnp.float32)
        part_ref[d] = total.astype(jnp.bfloat16)
        if i + depth < n_ep:
            fetch(i + depth).start()

    def incoming(v, j, coords):
        order = plans[v][0]
        out = []
        for l, frm, pred in tree_neighbors(place, order, j, coords):
            dim = order[l]
            side = jnp.where(frm > place.at[dim], 1, 0)
            out.append((stage_slot(dims, order, layouts[v], l, side, coords), pred))
        out.sort(key=lambda t: t[1] is not None)
        return out

    def await_slot(v, slot):
        ref = held[v].at[slot]
        pltpu.make_async_remote_copy(
            src_ref=ref, dst_ref=ref, send_sem=ssem.at[0], recv_sem=rsems[v].at[slot],
            device_id=(me, place.tp), device_id_type=MESH,
        ).wait_recv()

    def add(v, d, slots, final):
        _, first, count = plans[v]
        unit = 16 if count % 16 == 0 else count

        def some(i, carry):
            r = pl.multiple_of(i * unit, unit)
            at = pl.ds(first + r, unit)
            x = part_ref[d, at, :].astype(jnp.float32)
            for slot in slots:
                x = x + held[v][slot, pl.ds(r, unit), :].astype(jnp.float32)
            if final:
                mixed[at, :] = x
                y = x * x
                square = y[:, :LANES]
                for c in range(1, width // LANES):
                    square = square + y[:, c * LANES : (c + 1) * LANES]
                squares[at, :] = square
            else:
                part_ref[d, at, :] = x.astype(jnp.bfloat16)
            return carry

        lax.fori_loop(0, count // unit, some, 0)

    def collect_parts(v, d, inc, final):
        sure = [slot for slot, pred in inc if pred is None]
        unsure = [(slot, pred) for slot, pred in inc if pred is not None]
        for slot in sure:
            await_slot(v, slot)
        for slot, pred in unsure:
            maybe(pred, functools.partial(await_slot, v, slot))
        if not unsure:
            if sure or final:
                add(v, d, sure, final)
            return
        for picks in itertools.product((True, False), repeat=len(unsure)):
            cond = None
            for (_, pred), yes in zip(unsure, picks):
                term = pred if yes else jnp.logical_not(pred)
                cond = term if cond is None else cond & term
            slots = sure + [slot for (slot, _), yes in zip(unsure, picks) if yes]
            if slots or final:
                maybe(cond, functools.partial(add, v, d, slots, final))

    done = 0
    for v, j, ks in events:
        order, first, count = plans[v]
        coords = event_block(place, order, j, ks)
        d = place.flat(coords)
        while relative(plans, v, ks) not in needed[:done]:
            mix(done)
            done += 1
        collect_parts(v, d, incoming(v, j, coords), False)
        dim = order[j]
        m = place.at[dim]
        to = 1 - m if dims[dim] == 2 else m + jnp.where(coords[dim] > m, 1, -1)
        side = jnp.where(m > to, 1, 0)
        slot = stage_slot(dims, order, layouts[v], j, side, coords)
        copy = pltpu.make_async_remote_copy(
            src_ref=part_ref.at[d, pl.ds(first, count)],
            dst_ref=held[v].at[slot],
            send_sem=ssem.at[len(sends)],
            recv_sem=rsems[v].at[slot],
            device_id=(place.moved(dim, to), place.tp),
            device_id_type=MESH,
        )
        copy.start()
        sends.append(copy)
    while done < n_ep:
        mix(done)
        done += 1
    for v, (order, first, count) in enumerate(plans):
        collect_parts(v, me, incoming(v, -1, place.at), True)

    shares = []
    for o in range(1, n_tp):
        copy = pltpu.make_async_remote_copy(
            src_ref=squares,
            dst_ref=others.at[o],
            send_sem=ossem.at[o],
            recv_sem=orsem.at[o],
            device_id=(me, (place.tp + o) % n_tp),
            device_id_type=MESH,
        )
        copy.start()
        shares.append(copy)
    for copy in shares:
        copy.wait_recv()
    unit = 32

    def norm(i, carry):
        at = pl.ds(pl.multiple_of(i * unit, unit), unit)
        square = squares[at, :]
        for o in range(1, n_tp):
            square = square + others[o, at, :]
        power = jnp.sum(square, axis=1, keepdims=True) / (width * n_tp)
        out_ref[at, :] = (mixed[at, :] * lax.rsqrt(power + 1e-06) * gain_ref[...]).astype(jnp.bfloat16)
        return carry

    lax.fori_loop(0, tok_rows // unit, norm, 0)
    for copy in shares + sends:
        copy.wait_send()


def scatter_norm(coef, words, gain, rows, dims, plans, n_tp, tok_rows, lines):
    n_ep, cap, width = rows.shape
    counts = [(stage_layout(order, dims)[1], count) for order, _, count in plans]
    vmem = pl.BlockSpec(memory_space=pltpu.VMEM)
    depth = 3
    return pl.pallas_call(
        functools.partial(scatter_kernel, dims, plans, n_tp, lines),
        out_shape=jax.ShapeDtypeStruct((tok_rows, width), jnp.bfloat16),
        in_specs=[vmem, vmem, vmem, pl.BlockSpec(memory_space=pl.ANY)],
        out_specs=vmem,
        scratch_shapes=[
            pltpu.VMEM((n_ep, tok_rows, width), jnp.bfloat16),
            pltpu.VMEM((tok_rows, width), jnp.float32),
            pltpu.VMEM((tok_rows, LANES), jnp.float32),
            pltpu.VMEM((n_tp, tok_rows, LANES), jnp.float32),
            pltpu.VMEM((depth, cap, width), jnp.bfloat16),
        ]
        + [pltpu.VMEM((slots, count, width), jnp.bfloat16) for slots, count in counts]
        + [pltpu.SemaphoreType.DMA((slots,)) for slots, _ in counts]
        + [
            pltpu.SemaphoreType.DMA((depth,)),
            pltpu.SemaphoreType.DMA((n_tp,)),
            pltpu.SemaphoreType.DMA((n_tp,)),
            pltpu.SemaphoreType.DMA((len(schedule(plans, dims, ())),)),
        ],
        compiler_params=pltpu.CompilerParams(
            collective_id=1, has_side_effects=True, vmem_limit_bytes=VMEM_LIMIT
        ),
        name="scatter_norm",
    )(coef, words, gain, rows)


def body(dims, n_tp, tokens, experts, weights, up_table, out_table, gain):
    n_ep = int(np.prod(dims))
    tok_rows, width = tokens.shape
    cap = 2 * tok_rows * experts.shape[1] // n_ep
    plans = tree_plans(dims, tok_rows)
    rows_held = up_table.shape[0]
    my_words, my_weights = route(experts.T, weights.T, n_ep, cap, rows_held, width // LANES)
    coef, words, rows = collect(
        my_words, my_weights, tokens, up_table, out_table, dims, plans, n_tp, cap
    )
    return scatter_norm(
        coef, words, gain.reshape(1, width), rows, dims, plans, n_tp, tok_rows, lines_of(rows_held, width // LANES)
    )


def solution(mesh):
    placed = (P("ep", "tp"), P("ep", None), P("ep", None), P("ep", "tp"), P("ep", "tp"), P("tp"))
    return jax.shard_map(
        functools.partial(body, ep_dims(mesh), mesh.shape["tp"]),
        mesh=mesh,
        in_specs=placed,
        out_specs=P("ep", "tp"),
        check_vma=False,
    )
```

```python
import functools
import itertools

import jax
import jax.numpy as jnp
import numpy as np
from jax import lax
from jax.experimental import pallas as pl
from jax.experimental.pallas import tpu as pltpu
from jax.sharding import PartitionSpec as P

LANES = 128
MESH = pl.DeviceIdType.MESH
NT = (((1,), (1,)), ((), ()))
VMEM_LIMIT = 63 * 1024 * 1024
PITCH = 9
SPAN = 66.0
LOAD, TAKE, DOT = 0.35, 0.85, 0.65
DEPTH = 8
SCATTER_ORDER = ()
GATHER_ORDER = (
    0, 15, 1, 31, 30, 46, 45, 18, 48, 3, 49, 19, 16, 5, 36, 7, 11, 37, 51, 54, 47, 4, 32, 52, 33, 55,
    50, 39, 34, 20, 2, 17, 58, 42, 22, 25, 40, 57, 43, 6, 35, 41, 9, 12, 24, 53, 28, 21, 13, 26, 10, 44,
    59, 56, 8, 38, 27, 14, 23, 29,
)


def ep_dims(mesh):
    n = mesh.shape["ep"]
    devices = np.moveaxis(mesh.devices, mesh.axis_names.index("ep"), 0).reshape(n, -1)[:, 0]
    coords = [getattr(d, "coords", None) for d in devices]
    if any(c is None for c in coords):
        return (n,)
    axes = []
    for a in range(len(coords[0])):
        values = [c[a] for c in coords]
        size = len(set(values))
        if size > 1:
            stride = next(i for i in range(n) if values[i] != values[0])
            axes.append((stride, size, [v - min(values) for v in values]))
    axes.sort(key=lambda t: -t[0])
    dims = tuple(size for _, size, _ in axes)
    if int(np.prod(dims)) != n:
        return (n,)
    for i in range(n):
        if any((i // stride) % size != values[i] for stride, size, values in axes):
            return (n,)
    return dims


def tree_plans(dims, rows):
    k = len(dims)
    if k == 3 and rows % 128 == 0:
        long, mid, last = sorted(range(3), key=lambda i: -dims[i])
        unit = rows // 8
        plans = [
            ((long, mid, last), 3 * unit),
            ((long, last, mid), 3 * unit),
            ((last, mid, long), unit),
            ((mid, last, long), unit),
        ]
    elif k == 2 and rows % 32 == 0:
        plans = [((0, 1), rows // 2), ((1, 0), rows // 2)]
    else:
        plans = [(tuple(range(k)), rows)]
    out, first = [], 0
    for order, count in plans:
        out.append((order, first, count))
        first += count
    return out


class Place:
    def __init__(self, dims):
        self.dims = dims
        self.strides = [int(np.prod(dims[i + 1 :])) for i in range(len(dims))]
        self.e = lax.axis_index("ep")
        self.tp = lax.axis_index("tp")
        self.at = [(self.e // st) % n for st, n in zip(self.strides, dims)]

    def near(self, dim, k):
        m, n = self.at[dim], self.dims[dim]
        if k == 0:
            return m
        if n == 2:
            return 1 - m
        below, above = m, n - 1 - m
        low = jnp.minimum(below, above)
        hop = (k + 1) // 2
        alternate = m + hop if k % 2 else m - hop
        far = jnp.where(below < above, m + (k - low), m - (k - low))
        return jnp.where(k <= 2 * low, alternate, far)

    def flat(self, coords):
        total = 0
        for c, st in zip(coords, self.strides):
            total = total + c * st
        return total

    def moved(self, dim, to):
        return self.e + (to - self.at[dim]) * self.strides[dim]


def tree_events(order, dims):
    events = []
    for j in range(len(order)):
        heads = [range(dims[order[i]]) for i in range(j)] + [range(1, dims[order[j]])]
        for ks in itertools.product(*heads):
            events.append((j, ks))
    return events


def event_block(place, order, j, ks):
    coords = list(place.at)
    for i in range(j + 1):
        coords[order[i]] = place.near(order[i], ks[i])
    return coords


def tree_neighbors(place, order, j, coords):
    out = []
    for l in range(max(j, 0), len(order)):
        dim = order[l]
        n, m = place.dims[dim], place.at[dim]
        if l == j:
            if n > 2:
                to = m + jnp.where(m > coords[dim], 1, -1)
                out.append((l, to, (to >= 0) & (to < n)))
        elif n == 2:
            out.append((l, 1 - m, None))
        else:
            out.append((l, m + 1, m + 1 < n))
            out.append((l, m - 1, m > 0))
    return out


def schedule(plans, dims, table):
    keyed = []
    for v, (order, _, count) in enumerate(plans):
        seen = {}
        for j, ks in tree_events(order, dims):
            dist = sum((k + 1) // 2 if dims[order[i]] > 2 else k for i, k in enumerate(ks))
            before = seen.get(j, 0)
            seen[j] = before + 1
            keyed.append(((dist + before) * 1.0 + 0.01 * j, v, j, ks))
    events = [(v, j, ks) for _, v, j, ks in keyed]
    if len(events) == len(table):
        return [events[i] for i in table]
    keyed.sort(key=lambda t: t[0])
    return [(v, j, ks) for _, v, j, ks in keyed]


def relative(plans, v, ks):
    order = plans[v][0]
    ranks = [0] * len(order)
    for i, k in enumerate(ks):
        ranks[order[i]] = k
    return tuple(ranks)


def block_of(place, ranks):
    return place.flat([place.near(dim, k) for dim, k in enumerate(ranks)])


def maybe(pred, fn):
    if pred is None:
        fn()
    else:
        pl.when(pred)(fn)


def count_sends(plans, dims):
    total = 0
    for order, _, _ in plans:
        for j, _ in [(-1, ())] + tree_events(order, dims):
            for l in range(max(j, 0), len(order)):
                big = dims[order[l]] > 2
                total += (1 if big else 0) if l == j else (2 if big else 1)
    return total


def route_kernel(n_ep, cap, rows_held, sub, experts_ref, weights_ref, word_ref, weight_ref):
    slots, tok_rows = experts_ref.shape
    col = lax.broadcasted_iota(jnp.int32, (tok_rows, tok_rows), 1)
    row = lax.broadcasted_iota(jnp.int32, (tok_rows, tok_rows), 0)
    before = (row < col).astype(jnp.float32).astype(jnp.bfloat16)
    owners = lax.broadcasted_iota(jnp.int32, (n_ep, tok_rows), 0)
    places = lax.broadcasted_iota(jnp.int32, (cap, tok_rows), 0)
    token = lax.broadcasted_iota(jnp.int32, (1, tok_rows), 1)
    total = jnp.zeros((6 * n_ep, cap), jnp.float32)
    found = [(experts_ref[k : k + 1, :] // rows_held) == owners for k in range(slots)]
    ones = jnp.concatenate([jnp.where(mine, 1.0, 0.0) for mine in found], axis=0)
    ahead_all = jnp.dot(ones.astype(jnp.bfloat16), before, preferred_element_type=jnp.float32)
    sums = jnp.sum(ones, axis=1, keepdims=True)
    base = jnp.zeros((n_ep, 1), jnp.float32)
    for k in range(slots):
        e = experts_ref[k : k + 1, :]
        owner = e // rows_held
        mine = found[k]
        ahead = ahead_all[k * n_ep : (k + 1) * n_ep, :] + base
        base = base + sums[k * n_ep : (k + 1) * n_ep, :]
        rank = jnp.sum(jnp.where(mine, ahead, 0.0), axis=0, keepdims=True).astype(jnp.int32)
        at = jnp.where(rank == places, 1.0, 0.0).astype(jnp.bfloat16)
        word = token * rows_held + (e - owner * rows_held)
        w = weights_ref[k : k + 1, :]
        w0 = w.astype(jnp.bfloat16).astype(jnp.float32)
        w1 = (w - w0).astype(jnp.bfloat16).astype(jnp.float32)
        w2 = w - w0 - w1
        parts = [(word & 255), ((word >> 8) & 255), (word >> 16)]
        parts = [p.astype(jnp.float32) for p in parts] + [w0, w1, w2]
        lhs = jnp.concatenate([jnp.where(mine, p, 0.0) for p in parts], axis=0).astype(jnp.bfloat16)
        total = total + lax.dot_general(lhs, at, NT, preferred_element_type=jnp.float32)
    take = lambda i: total[i * n_ep : (i + 1) * n_ep, :]
    word = (take(0) + 256.0 * take(1) + 65536.0 * take(2)).astype(jnp.int32)
    token = word // rows_held
    row = word - token * rows_held
    line = (row // 8) * (sub * PITCH - 8) + row
    word_ref[:, 0, :] = token * lines_of(rows_held, sub) + line
    weight_ref[:, 0, :] = take(3) + take(4) + take(5)


def lines_of(rows_held, sub):
    return rows_held // 8 * sub * PITCH


def route(experts_t, weights_t, n_ep, cap, rows_held, sub):
    lists = (n_ep, 1, cap)
    return pl.pallas_call(
        functools.partial(route_kernel, n_ep, cap, rows_held, sub),
        out_shape=(jax.ShapeDtypeStruct(lists, jnp.int32), jax.ShapeDtypeStruct(lists, jnp.float32)),
        name="route",
    )(experts_t, weights_t)


def table_piece(table_ref, flat, stage, sem, i, slot):
    step, width = stage.shape[1:]
    sub = width // LANES
    copy = pltpu.make_async_copy(table_ref.at[pl.ds(i * step, step)], stage.at[slot], sem.at[slot])

    def rest():
        copy.wait()

        def spread(g, carry):
            r = pl.multiple_of(g * 16, 16)
            for c in range(sub):
                x = stage[slot, pl.ds(r, 16), c * LANES : (c + 1) * LANES].astype(jnp.float32)
                for h in range(2):
                    first = ((i * (step // 8) + g * 2 + h) * sub + c) * PITCH
                    flat[pl.ds(first, 8), :] = x[8 * h : 8 * h + 8, :]
            return carry

        lax.fori_loop(0, step // 16, spread, 0)

    return copy.start, rest


def take_rows(row_ref, s, cap, sub, flat, picked, put):
    batch = 32
    gap = sub + 1 if sub > 1 else 1
    groups = cap // LANES

    def some(q, carry):
        for g in range(LANES // batch):
            taken = []
            for u in range(batch):
                at = row_ref[s * groups + q, g * batch + u]
                taken.append(flat[pl.ds(at, sub, stride=PITCH), :] if sub > 1 else flat[pl.ds(at, 1), :])
            for u in range(batch):
                picked[pl.ds((q * LANES + g * batch + u) * gap, sub), :] = taken[u]
        return carry

    lax.fori_loop(0, groups, some, 0)
    for c in range(sub):
        lines = picked[pl.ds(c, cap, stride=gap), :] if sub > 1 else picked[...]
        put(c, lines.astype(jnp.bfloat16))


def collect_kernel(
    dims, plans, n_tp, my_word, my_weight, tok_ref, up_ref, out_ref,
    coef_ref, word_ref, rows_ref,
    all_ref, weight_ref, row_held, row_ref, stage, flat, picked, packed, held, dots, others,
    ssem, rsem, wssem, wrsem, ossem, orsem, stage_sem, put_sem, row_sem,
):
    place = Place(dims)
    me = place.e
    n_ep, tok_rows, width = all_ref.shape
    cap = coef_ref.shape[2]
    rows_held = up_ref.shape[0]
    sub = width // LANES
    lines = lines_of(rows_held, sub)
    pieces = rows_held // stage.shape[1]
    depth = min(stage.shape[0], pieces)
    loads = [
        table_piece(table, flat, stage, stage_sem, i, i % depth) for table in (out_ref, up_ref) for i in range(pieces)
    ]
    for i in range(depth):
        loads[i][0]()

    barrier = pltpu.get_barrier_semaphore()
    for o in range(1, n_ep):
        pl.semaphore_signal(barrier, inc=1, device_id=((me + o) % n_ep, place.tp), device_id_type=MESH)
    for o in range(1, n_tp):
        pl.semaphore_signal(barrier, inc=1, device_id=(me, (place.tp + o) % n_tp), device_id_type=MESH)
    pl.semaphore_wait(barrier, n_ep + n_tp - 2)

    sends = []

    def forward(v, j, coords, src):
        order, first, count = plans[v]
        s = place.flat(coords)
        for l, to, pred in tree_neighbors(place, order, j, coords):
            copy = pltpu.make_async_remote_copy(
                src_ref=src,
                dst_ref=all_ref.at[s, pl.ds(first, count)],
                send_sem=ssem.at[len(sends)],
                recv_sem=rsem.at[v, s],
                device_id=(place.moved(order[l], to), place.tp),
                device_id_type=MESH,
            )
            maybe(pred, copy.start)
            sends.append((pred, copy))

    list_copies = []
    for o in range(1, n_ep):
        to = (me + o) % n_ep
        for i, (src, dst) in enumerate(((my_word, word_ref), (my_weight, weight_ref))):
            copy = pltpu.make_async_remote_copy(
                src_ref=src.at[to],
                dst_ref=dst.at[me],
                send_sem=wssem.at[i, o],
                recv_sem=wrsem.at[i, o],
                device_id=(to, place.tp),
                device_id_type=MESH,
            )
            copy.start()
            list_copies.append(copy)
    for v, (order, first, count) in enumerate(plans):
        forward(v, -1, place.at, tok_ref.at[pl.ds(first, count)])
    word_ref[me] = my_word[me]
    weight_ref[me] = my_weight[me]

    def load(i):
        loads[i][1]()
        if i + depth < len(loads):
            loads[i + depth][0]()

    def lists():
        for copy in list_copies:
            copy.wait_recv()
        for s in range(n_ep):
            word = word_ref[s]
            word = word - (word // lines) * lines
            for q in range(cap // LANES):
                at = s * (cap // LANES) + q
                row_held[at : at + 1, :] = word[:, q * LANES : (q + 1) * LANES]
        copy = pltpu.make_async_copy(row_held, row_ref, row_sem)
        copy.start()
        copy.wait()

    def put_copy(s):
        return pltpu.make_async_copy(packed.at[s % 2], rows_ref.at[s], put_sem.at[s % 2])

    def out_rows(s):
        if s >= 2:
            put_copy(s - 2).wait()

        def put(c, lines):
            packed[s % 2, :, c * LANES : (c + 1) * LANES] = lines

        take_rows(row_ref, s, cap, sub, flat, picked, put)
        put_copy(s).start()

    def up_rows(s):
        def put(c, lines):
            held[s, :, c * LANES : (c + 1) * LANES] = lines

        take_rows(row_ref, s, cap, sub, flat, picked, put)

    def dot_of(ranks):
        s = block_of(place, ranks)
        tok = tok_ref[...] if not any(ranks) else all_ref[s]
        full = lax.dot_general(tok, held[s], NT, preferred_element_type=jnp.float32)
        hit = (word_ref[s] // lines) == lax.broadcasted_iota(jnp.int32, (tok_rows, cap), 0)
        dots[s] = jnp.sum(jnp.where(hit, full, 0.0), axis=0, keepdims=True)

    events = schedule(plans, dims, GATHER_ORDER)
    last = {}
    for i, (v, j, ks) in enumerate(events):
        last[relative(plans, v, ks)] = i
    work = [(LOAD, functools.partial(load, i)) for i in range(pieces)] + [(0.5, lists)]
    work += [(TAKE, functools.partial(out_rows, s)) for s in range(n_ep)]
    work += [(LOAD, functools.partial(load, pieces + i)) for i in range(pieces)]
    work += [(TAKE, functools.partial(up_rows, s)) for s in range(n_ep)]
    ready = [(0,) * len(dims)]
    clock, per_event = 3.0, SPAN / len(events)
    for i, (v, j, ks) in enumerate(events):
        due = 4.0 + per_event * i
        while clock < due and (work or ready):
            if work:
                cost, fn = work.pop(0)
                fn()
                clock += cost
            else:
                dot_of(ready.pop(0))
                clock += DOT
        clock = max(clock, due)
        order, first, count = plans[v]
        coords = event_block(place, order, j, ks)
        s = place.flat(coords)
        block = all_ref.at[s, pl.ds(first, count)]
        pltpu.make_async_remote_copy(
            src_ref=block, dst_ref=block, send_sem=ssem.at[0], recv_sem=rsem.at[v, s],
            device_id=(me, place.tp), device_id_type=MESH,
        ).wait_recv()
        forward(v, j, coords, block)
        ranks = relative(plans, v, ks)
        if last[ranks] == i:
            ready.append(ranks)
    for _, fn in work:
        fn()
    for ranks in ready:
        dot_of(ranks)

    shares = []
    for o in range(1, n_tp):
        copy = pltpu.make_async_remote_copy(
            src_ref=dots,
            dst_ref=others.at[o],
            send_sem=ossem.at[o],
            recv_sem=orsem.at[o],
            device_id=(me, (place.tp + o) % n_tp),
            device_id_type=MESH,
        )
        copy.start()
        shares.append(copy)
    for copy in shares:
        copy.wait_recv()

    def finish(s, carry):
        dot = dots[s]
        for o in range(1, n_tp):
            dot = dot + others[o, s]
        coef_ref[s] = weight_ref[s] * jax.nn.gelu(dot)
        return carry

    lax.fori_loop(0, n_ep, finish, 0)
    for copy in shares + list_copies:
        copy.wait_send()
    for s in range(max(0, n_ep - 2), n_ep):
        put_copy(s).wait()
    for pred, copy in sends:
        maybe(pred, copy.wait_send)


def collect(words, weights, tokens, up_table, out_table, dims, plans, n_tp, cap):
    n_ep = int(np.prod(dims))
    tok_rows, width = tokens.shape
    rows_held = up_table.shape[0]
    sub = width // LANES
    vmem = pl.BlockSpec(memory_space=pltpu.VMEM)
    hbm = pl.BlockSpec(memory_space=pl.ANY)
    lists = (n_ep, 1, cap)
    return pl.pallas_call(
        functools.partial(collect_kernel, dims, plans, n_tp),
        out_shape=(
            jax.ShapeDtypeStruct(lists, jnp.float32),
            jax.ShapeDtypeStruct(lists, jnp.int32),
            jax.ShapeDtypeStruct((n_ep, cap, width), jnp.bfloat16),
        ),
        in_specs=[vmem, vmem, vmem, hbm, hbm],
        out_specs=(vmem, vmem, hbm),
        scratch_shapes=[
            pltpu.VMEM((n_ep, tok_rows, width), jnp.bfloat16),
            pltpu.VMEM(lists, jnp.float32),
            pltpu.VMEM((n_ep * cap // LANES, LANES), jnp.int32),
            pltpu.SMEM((n_ep * cap // LANES, LANES), jnp.int32),
            pltpu.VMEM((DEPTH, min(rows_held, 256), width), jnp.bfloat16),
            pltpu.VMEM((lines_of(rows_held, sub), LANES), jnp.float32),
            pltpu.VMEM((cap * (sub + 1 if sub > 1 else 1), LANES), jnp.float32),
            pltpu.VMEM((2, cap, width), jnp.bfloat16),
            pltpu.VMEM((n_ep, cap, width), jnp.bfloat16),
            pltpu.VMEM(lists, jnp.float32),
            pltpu.VMEM((n_tp,) + lists, jnp.float32),
            pltpu.SemaphoreType.DMA((count_sends(plans, dims),)),
            pltpu.SemaphoreType.DMA((len(plans), n_ep)),
            pltpu.SemaphoreType.DMA((2, n_ep)),
            pltpu.SemaphoreType.DMA((2, n_ep)),
            pltpu.SemaphoreType.DMA((n_tp,)),
            pltpu.SemaphoreType.DMA((n_tp,)),
            pltpu.SemaphoreType.DMA((DEPTH,)),
            pltpu.SemaphoreType.DMA((2,)),
            pltpu.SemaphoreType.DMA,
        ],
        compiler_params=pltpu.CompilerParams(
            collective_id=0, has_side_effects=True, vmem_limit_bytes=VMEM_LIMIT
        ),
        name="collect",
    )(words, weights, tokens, up_table, out_table)


def stage_layout(order, dims):
    bases, base = [], 0
    for j, dim in enumerate(order):
        bases.append(base)
        inner = int(np.prod([dims[order[i]] for i in range(j)]))
        base += (2 * dims[dim] if dims[dim] > 2 else 1) * inner
    return bases, base


def stage_slot(dims, order, bases, j, side, coords):
    n = dims[order[j]]
    inner, width = 0, 1
    for i in reversed(range(j)):
        inner = inner + coords[order[i]] * width
        width *= dims[order[i]]
    outer = (side * n + coords[order[j]]) if n > 2 else 0
    return bases[j] + outer * width + inner


def scatter_kernel(dims, plans, n_tp, lines, coef_ref, word_ref, gain_ref, rows_ref, out_ref, part_ref, mixed, squares, others, rows, *scratch):
    held = scratch[: len(plans)]
    rsems = scratch[len(plans) : 2 * len(plans)]
    row_sem, ossem, orsem, ssem = scratch[-4:]
    place = Place(dims)
    me = place.e
    n_ep, tok_rows, width = part_ref.shape
    cap = coef_ref.shape[2]
    events = list(reversed(schedule(plans, dims, SCATTER_ORDER)))
    needed = []
    for v, j, ks in events:
        ranks = relative(plans, v, ks)
        if ranks not in needed:
            needed.append(ranks)
    needed.append((0,) * len(dims))
    depth = rows.shape[0]

    def fetch(i):
        return pltpu.make_async_copy(rows_ref.at[block_of(place, needed[i])], rows.at[i % depth], row_sem.at[i % depth])

    for i in range(min(depth, n_ep)):
        fetch(i).start()
    barrier = pltpu.get_barrier_semaphore()
    around = []
    for dim, n in enumerate(dims):
        m = place.at[dim]
        if n == 2:
            around.append((place.moved(dim, 1 - m), None))
        else:
            around.append((place.moved(dim, m + 1), m + 1 < n))
            around.append((place.moved(dim, m - 1), m > 0))
    for to, pred in around:
        def greet(to=to):
            pl.semaphore_signal(barrier, inc=1, device_id=(to, place.tp), device_id_type=MESH)
        maybe(pred, greet)
    for o in range(1, n_tp):
        pl.semaphore_signal(barrier, inc=1, device_id=(me, (place.tp + o) % n_tp), device_id_type=MESH)
    met = sum(1 if pred is None else jnp.where(pred, 1, 0) for _, pred in around)
    pl.semaphore_wait(barrier, met + n_tp - 1)

    layouts = [stage_layout(order, dims)[0] for order, _, _ in plans]
    sends = []

    def mix(i):
        d = block_of(place, needed[i])
        fetch(i).wait()
        hit = (word_ref[d] // lines) == lax.broadcasted_iota(jnp.int32, (tok_rows, cap), 0)
        coef = coef_ref[d]
        high = coef.astype(jnp.bfloat16).astype(jnp.float32)
        low = coef - high
        table_rows = rows[i % depth]
        total = jnp.dot(jnp.where(hit, high, 0.0).astype(jnp.bfloat16), table_rows, preferred_element_type=jnp.float32)
        total += jnp.dot(jnp.where(hit, low, 0.0).astype(jnp.bfloat16), table_rows, preferred_element_type=jnp.float32)
        part_ref[d] = total.astype(jnp.bfloat16)
        if i + depth < n_ep:
            fetch(i + depth).start()

    def incoming(v, j, coords):
        order = plans[v][0]
        out = []
        for l, frm, pred in tree_neighbors(place, order, j, coords):
            dim = order[l]
            side = jnp.where(frm > place.at[dim], 1, 0)
            out.append((stage_slot(dims, order, layouts[v], l, side, coords), pred))
        out.sort(key=lambda t: t[1] is not None)
        return out

    def await_slot(v, slot):
        ref = held[v].at[slot]
        pltpu.make_async_remote_copy(
            src_ref=ref, dst_ref=ref, send_sem=ssem.at[0], recv_sem=rsems[v].at[slot],
            device_id=(me, place.tp), device_id_type=MESH,
        ).wait_recv()

    def add(v, d, slots, final):
        _, first, count = plans[v]
        unit = 16 if count % 16 == 0 else count

        def some(i, carry):
            r = pl.multiple_of(i * unit, unit)
            at = pl.ds(first + r, unit)
            x = part_ref[d, at, :].astype(jnp.float32)
            for slot in slots:
                x = x + held[v][slot, pl.ds(r, unit), :].astype(jnp.float32)
            if final:
                mixed[at, :] = x
                y = x * x
                square = y[:, :LANES]
                for c in range(1, width // LANES):
                    square = square + y[:, c * LANES : (c + 1) * LANES]
                squares[at, :] = square
            else:
                part_ref[d, at, :] = x.astype(jnp.bfloat16)
            return carry

        lax.fori_loop(0, count // unit, some, 0)

    def collect_parts(v, d, inc, final):
        sure = [slot for slot, pred in inc if pred is None]
        unsure = [(slot, pred) for slot, pred in inc if pred is not None]
        for slot in sure:
            await_slot(v, slot)
        for slot, pred in unsure:
            maybe(pred, functools.partial(await_slot, v, slot))
        if not unsure:
            if sure or final:
                add(v, d, sure, final)
            return
        for picks in itertools.product((True, False), repeat=len(unsure)):
            cond = None
            for (_, pred), yes in zip(unsure, picks):
                term = pred if yes else jnp.logical_not(pred)
                cond = term if cond is None else cond & term
            slots = sure + [slot for (slot, _), yes in zip(unsure, picks) if yes]
            if slots or final:
                maybe(cond, functools.partial(add, v, d, slots, final))

    done = 0
    for v, j, ks in events:
        order, first, count = plans[v]
        coords = event_block(place, order, j, ks)
        d = place.flat(coords)
        while relative(plans, v, ks) not in needed[:done]:
            mix(done)
            done += 1
        collect_parts(v, d, incoming(v, j, coords), False)
        dim = order[j]
        m = place.at[dim]
        to = 1 - m if dims[dim] == 2 else m + jnp.where(coords[dim] > m, 1, -1)
        side = jnp.where(m > to, 1, 0)
        slot = stage_slot(dims, order, layouts[v], j, side, coords)
        copy = pltpu.make_async_remote_copy(
            src_ref=part_ref.at[d, pl.ds(first, count)],
            dst_ref=held[v].at[slot],
            send_sem=ssem.at[len(sends)],
            recv_sem=rsems[v].at[slot],
            device_id=(place.moved(dim, to), place.tp),
            device_id_type=MESH,
        )
        copy.start()
        sends.append(copy)
    while done < n_ep:
        mix(done)
        done += 1
    for v, (order, first, count) in enumerate(plans):
        collect_parts(v, me, incoming(v, -1, place.at), True)

    shares = []
    for o in range(1, n_tp):
        copy = pltpu.make_async_remote_copy(
            src_ref=squares,
            dst_ref=others.at[o],
            send_sem=ossem.at[o],
            recv_sem=orsem.at[o],
            device_id=(me, (place.tp + o) % n_tp),
            device_id_type=MESH,
        )
        copy.start()
        shares.append(copy)
    for copy in shares:
        copy.wait_recv()
    unit = 32

    def norm(i, carry):
        at = pl.ds(pl.multiple_of(i * unit, unit), unit)
        square = squares[at, :]
        for o in range(1, n_tp):
            square = square + others[o, at, :]
        power = jnp.sum(square, axis=1, keepdims=True) / (width * n_tp)
        out_ref[at, :] = (mixed[at, :] * lax.rsqrt(power + 1e-06) * gain_ref[...]).astype(jnp.bfloat16)
        return carry

    lax.fori_loop(0, tok_rows // unit, norm, 0)
    for copy in shares + sends:
        copy.wait_send()


def scatter_norm(coef, words, gain, rows, dims, plans, n_tp, tok_rows, lines):
    n_ep, cap, width = rows.shape
    counts = [(stage_layout(order, dims)[1], count) for order, _, count in plans]
    vmem = pl.BlockSpec(memory_space=pltpu.VMEM)
    depth = 3
    return pl.pallas_call(
        functools.partial(scatter_kernel, dims, plans, n_tp, lines),
        out_shape=jax.ShapeDtypeStruct((tok_rows, width), jnp.bfloat16),
        in_specs=[vmem, vmem, vmem, pl.BlockSpec(memory_space=pl.ANY)],
        out_specs=vmem,
        scratch_shapes=[
            pltpu.VMEM((n_ep, tok_rows, width), jnp.bfloat16),
            pltpu.VMEM((tok_rows, width), jnp.float32),
            pltpu.VMEM((tok_rows, LANES), jnp.float32),
            pltpu.VMEM((n_tp, tok_rows, LANES), jnp.float32),
            pltpu.VMEM((depth, cap, width), jnp.bfloat16),
        ]
        + [pltpu.VMEM((slots, count, width), jnp.bfloat16) for slots, count in counts]
        + [pltpu.SemaphoreType.DMA((slots,)) for slots, _ in counts]
        + [
            pltpu.SemaphoreType.DMA((depth,)),
            pltpu.SemaphoreType.DMA((n_tp,)),
            pltpu.SemaphoreType.DMA((n_tp,)),
            pltpu.SemaphoreType.DMA((len(schedule(plans, dims, ())),)),
        ],
        compiler_params=pltpu.CompilerParams(
            collective_id=1, has_side_effects=True, vmem_limit_bytes=VMEM_LIMIT
        ),
        name="scatter_norm",
    )(coef, words, gain, rows)


def body(dims, n_tp, tokens, experts, weights, up_table, out_table, gain):
    n_ep = int(np.prod(dims))
    tok_rows, width = tokens.shape
    cap = 2 * tok_rows * experts.shape[1] // n_ep
    plans = tree_plans(dims, tok_rows)
    rows_held = up_table.shape[0]
    my_words, my_weights = route(experts.T, weights.T, n_ep, cap, rows_held, width // LANES)
    coef, words, rows = collect(
        my_words, my_weights, tokens, up_table, out_table, dims, plans, n_tp, cap
    )
    return scatter_norm(
        coef, words, gain.reshape(1, width), rows, dims, plans, n_tp, tok_rows, lines_of(rows_held, width // LANES)
    )


def solution(mesh):
    placed = (P("ep", "tp"), P("ep", None), P("ep", None), P("ep", "tp"), P("ep", "tp"), P("tp"))
    return jax.shard_map(
        functools.partial(body, ep_dims(mesh), mesh.shape["tp"]),
        mesh=mesh,
        in_specs=placed,
        out_specs=P("ep", "tp"),
        check_vma=False,
    )
```
